256 devices in a mesh: sp: 64 (over z, x, core), tp: 4 (over y).
Axes of the slice: x: 4, y: 4, z: 8, core: 2. Of those that a mesh axis runs over, the one named last changes fastest.
Arguments:
- queries: bfloat16 [16384, 1024], P('sp', 'tp'), may hold values from -6 to 6
- keys: bfloat16 [16384, 1024], P('sp', 'tp'), may hold values from -72 to 72
- values: bfloat16 [16384, 1024], P('sp', 'tp'), may hold values from -6 to 6
- score_offset: float32 [8], P('tp'), may hold values from 2 to 11
- head_gain: float32 [128], replicated, may hold values from 0.1 to 1.9
- out_weight: bfloat16 [1024, 2048], P('tp'), may hold values from -0.1875 to 0.1875
- residual: bfloat16 [16384, 2048], P(('sp', 'tp')), may hold values from -6 to 6
- ln1_gain: float32 [2048], replicated, may hold values from 0.1 to 1.9
- ln1_bias: float32 [2048], replicated, may hold values from -2.5 to 2.5
- expert_ids: int32 [16384, 2], P(('sp', 'tp')), may hold values from 0 to 63, all different within a row; in each aligned block of 64 rows (0 to 63, 64 to 127, ...) at most 4 rows name the same one
- route_logits: float32 [16384, 2], P(('sp', 'tp')), may hold values from -6 to 6
- gate_weight: bfloat16 [64, 2048, 3072], P('sp', None, 'tp'), may hold values from -0.125 to 0.125
- up_weight: bfloat16 [64, 2048, 3072], P('sp', None, 'tp'), may hold values from -0.125 to 0.125
- down_weight: bfloat16 [64, 3072, 2048], P('sp', 'tp'), may hold values from -0.109375 to 0.109375
- ln2_gain: float32 [2048], replicated, may hold values from 0.1 to 1.9
- ln2_bias: float32 [2048], replicated, may hold values from -2.5 to 2.5
Outputs:
- output: bfloat16 [16384, 2048], P(('sp', 'tp'))
The draws below stay inside these ranges and needn't reach their ends.
Inputs may be any that keep to these rules, and one draw needn't show every extreme that they name: `expert_ids`: each row names 2 different experts. In the rows of one device no expert is named by more than 4 rows, and in every draw some expert is named by exactly 4 rows of some device.
All inputs are finite; a program needn't handle non-finite values.
Results may differ from the reference program's by a relative error of at most 0.012.
Values may be sent and summed in bfloat16 or wider, within the bound.
No kernel may reach another device: no remote copies, remote signals or barrier semaphores. Data moves between devices by JAX's collectives and lax.ppermute only.
A program may use at most 128 MiB of HBM per device.

```python
import math
import jax
import jax.numpy as jnp
import numpy as np
from jax import lax

D = 2048
HEADS = 8
HD = 128
FF = 3072
TOP = 2
TOK_DEV = 256
SB_WIDTH = 1024
SEQUENCE_TOKENS = 16384
EXPERTS = 64
CAP = 4
N_SP = 64
N_TP = 4


def draw_keys(key, part):
    starting_key, key_for_block, spike_key = jax.random.split(key, 3)
    base = jnp.clip(jax.random.normal(starting_key, (SEQUENCE_TOKENS, SB_WIDTH), jnp.float32), -6.0, 6.0)
    low_scale = 0.6
    high_scale = 1.5
    blocks = jnp.exp(jax.random.uniform(key_for_block, (SEQUENCE_TOKENS // TOK_DEV,), jnp.float32, jnp.log(low_scale), jnp.log(high_scale)))
    row_scale = jnp.repeat(blocks, TOK_DEV)
    spike_position = jax.random.randint(spike_key, (8,), 0, SEQUENCE_TOKENS)
    spiking_flag = jnp.any(jnp.arange(SEQUENCE_TOKENS)[:, None] == spike_position[None, :], axis=1)
    row_scale = jnp.where(spiking_flag, 12.0, row_scale)
    return (base * row_scale[:, None]).astype(jnp.bfloat16)


def draw_score_offset(key, part):
    pick_key, fast_key, slow_key = jax.random.split(key, 3)
    slow_value = jax.random.uniform(slow_key, (HEADS,), jnp.float32, 9.5, 11.0)
    fast_value = jax.random.uniform(fast_key, (HEADS,), jnp.float32, 2.0, 4.0)
    slow_heads = jax.random.randint(pick_key, (HEADS,), 0, 2) == 1
    return jnp.where(slow_heads, slow_value, fast_value)


def block_levels(own_key, dims, pieces, least, top_value):
    loudness = 1.0
    for dim, parts in pieces:
        heights = jax.random.uniform(jax.random.fold_in(jax.random.fold_in(own_key, 6), dim), (parts,), jnp.float32, least / len(pieces), top_value / len(pieces))
        loudness = loudness * jnp.repeat(jnp.exp(heights), dims[dim] // parts).reshape((-1,) + (1,) * (len(dims) - 1 - dim))
    return loudness


def deal_out(key, own, number, rows, number_of, top, most, skew):
    order = jax.random.permutation(key, number_of)
    heavy_load, ordinary = portions_of(number_of, rows * top, most, skew, True), portions_of(number_of, rows * top, most, skew, False)
    places = jnp.arange(number_of)

    def named(tallies, rotation):
        used = int((tallies > 0).sum())
        fixed = max(1, used // 4)
        moved = fixed + (places - fixed + rotation * (used - fixed)) % max(1, number_of - fixed)
        return jnp.zeros((number_of,), jnp.int32).at[order[jnp.where(places < fixed, places, moved)]].set(jnp.asarray(tallies, jnp.int32))

    tallies = jnp.where(number % 4 == 0, named(heavy_load, number // 4), named(ordinary, number - number // 4 - 1))
    mixed = jax.random.permutation(jax.random.fold_in(own, 3), number_of)
    donor, receiver = mixed[0:number_of // 2 * 2:2], mixed[1:number_of // 2 * 2:2]
    room = jnp.minimum(tallies[donor] - 1, most - tallies[receiver]) // 2
    room = jnp.where((donor == order[0]) | (receiver == order[0]) | (tallies[receiver] == 0), 0, jnp.maximum(room, 0))
    moved = jax.random.randint(jax.random.fold_in(own, 4), (number_of // 2,), 0, 1 << 20) % (room + 1)
    tallies = tallies.at[donor].add(-moved).at[receiver].add(moved)
    members = jnp.searchsorted(jnp.cumsum(tallies), jnp.arange(rows * top), side="right").astype(jnp.int32)
    listing = members.reshape(top, rows).T
    listing = listing[jax.random.permutation(jax.random.fold_in(own, 1), rows)]
    rotation = jax.random.randint(jax.random.fold_in(own, 2), (rows, 1), 0, top)
    return jnp.take_along_axis(listing, (jnp.arange(top)[None, :] + rotation) % top, axis=1)


def portions_of(number_of, total, reach, lean, full):
    portions = [(1 << 20) // math.isqrt(grade ** lean) + 1 for grade in range(1, number_of + 1)]
    largest = reach if full else min(reach, max(-(-total // number_of), total * portions[0] // sum(portions)))
    least = 1 if total - largest >= number_of - 1 else 0
    given, rest = [largest] + [least] * (number_of - 1), total - largest - least * (number_of - 1)
    while rest > 0:
        free = [i for i in range(1, number_of) if given[i] < largest] or [i for i in range(1, number_of) if given[i] < reach]
        whole, remaining = sum([portions[i] for i in free]), rest
        for i in free:
            extra = min(reach - given[i], max(1, remaining * portions[i] // whole), rest)
            given[i] = given[i] + extra
            rest = rest - extra
    return np.array(given)


def bell_draw(rng, dims, spread, bound, shards=(), kind=jnp.bfloat16):
    level = block_levels(rng, dims, shards, -0.22, 0.18) if shards else 1.0
    array = jax.random.normal(rng, dims, jnp.float32) * spread * level
    return jnp.minimum(jnp.maximum(array, -bound), bound).astype(kind)


def setup_inputs(seed: int = 0) -> dict:
    seeds = jax.random.split(jax.random.key(seed), 17)
    queries = bell_draw(seeds[0], (SEQUENCE_TOKENS, SB_WIDTH), 1.0, 6.0, ((0, 64), (1, 4)))
    keys = draw_keys(jax.random.fold_in(seeds[16], 71), 0)
    values = bell_draw(seeds[2], (SEQUENCE_TOKENS, SB_WIDTH), 1.0, 6.0, ((0, 64), (1, 4)))
    score_offset = draw_score_offset(jax.random.fold_in(seeds[16], 71), 0)
    head_gain = jnp.clip(1.0 + 0.18 * jax.random.normal(seeds[4], (HD,), jnp.float32), 0.1, 1.9)
    out_weight = bell_draw(seeds[5], (SB_WIDTH, D), SB_WIDTH ** -0.5, 0.1875, ((0, 4),))
    residual = bell_draw(seeds[6], (SEQUENCE_TOKENS, D), 1.0, 6.0, ((0, 256),))
    ln1_gain = jnp.clip(1.0 + 0.18 * jax.random.normal(seeds[7], (D,), jnp.float32), 0.1, 1.9)
    ln1_bias = bell_draw(seeds[8], (D,), 0.3, 2.5, (), jnp.float32)
    expert_ids_keys = jax.random.split(jax.random.fold_in(seeds[9], 1), SEQUENCE_TOKENS // (TOK_DEV // N_TP))
    expert_ids_turns = jax.random.permutation(jax.random.fold_in(seeds[9], 3), SEQUENCE_TOKENS // (TOK_DEV // N_TP))
    expert_ids = jax.vmap(lambda own, number: deal_out(jax.random.fold_in(seeds[9], 2), own, number, TOK_DEV // N_TP, EXPERTS, TOP, CAP, 1))(expert_ids_keys, expert_ids_turns).reshape((SEQUENCE_TOKENS, TOP))
    route_logits = bell_draw(seeds[10], (SEQUENCE_TOKENS, TOP), 1.5, 6.0, ((0, 256),), jnp.float32)
    gate_weight = bell_draw(seeds[11], (EXPERTS, D, FF), D ** -0.5, 0.125, ((0, 64), (2, 4)))
    up_weight = bell_draw(seeds[12], (EXPERTS, D, FF), D ** -0.5, 0.125, ((0, 64), (2, 4)))
    down_weight = bell_draw(seeds[13], (EXPERTS, FF, D), FF ** -0.5, 0.109375, ((0, 64), (1, 4)))
    ln2_gain = jnp.clip(1.0 + 0.18 * jax.random.normal(seeds[14], (D,), jnp.float32), 0.1, 1.9)
    ln2_bias = bell_draw(seeds[15], (D,), 0.3, 2.5, (), jnp.float32)
    return {"queries": queries, "keys": keys, "values": values, "score_offset": score_offset, "head_gain": head_gain, "out_weight": out_weight, "residual": residual, "ln1_gain": ln1_gain, "ln1_bias": ln1_bias, "expert_ids": expert_ids, "route_logits": route_logits, "gate_weight": gate_weight, "up_weight": up_weight, "down_weight": down_weight, "ln2_gain": ln2_gain, "ln2_bias": ln2_bias}


residual_scale = 8.0 ** 0.25
norm_eps = 1e-05
head_eps = 1e-06

def layer_norm(inputs, gain, shift):
    mean_value = lax.optimization_barrier(jnp.mean(inputs, axis=-1, keepdims=True))
    centred = inputs - mean_value
    variance = lax.optimization_barrier(jnp.mean(centred * centred, axis=-1, keepdims=True))
    return centred * lax.rsqrt(variance + norm_eps) * gain + shift

def reference(queries, keys, values, score_offset, head_gain, out_weight, residual, ln1_gain, ln1_bias, expert_ids, route_logits, gate_weight, up_weight, down_weight, ln2_gain, ln2_bias):
    query_heads = queries.astype(jnp.float32).reshape(SEQUENCE_TOKENS, HEADS, HD)
    key_heads = keys.astype(jnp.float32).reshape(SEQUENCE_TOKENS, HEADS, HD)
    value_heads = values.astype(jnp.float32).reshape(SEQUENCE_TOKENS, HEADS, HD)
    block_rows = math.gcd(SEQUENCE_TOKENS, 256)
    key_pos = jnp.arange(SEQUENCE_TOKENS, dtype=jnp.int32)
    scale = HD ** (-0.5)

    def one_block(begin):
        block_queries = lax.dynamic_slice_in_dim(query_heads, begin, block_rows, 0)
        scores = jnp.einsum('qhd,khd->hqk', block_queries, key_heads) * scale - score_offset[:, None, None]
        query_pos = begin + jnp.arange(block_rows, dtype=jnp.int32)
        causal = (key_pos[None, :] < query_pos[:, None])[None]
        log_keep = jnp.where(causal, jax.nn.log_sigmoid(-scores), 0.0)
        tail_sum = lax.cumsum(log_keep, axis=2, reverse=True) - log_keep
        stick = jnp.where(causal, jnp.exp(jax.nn.log_sigmoid(scores) + tail_sum), 0.0)
        rounded = lax.optimization_barrier(stick.astype(jnp.bfloat16)).astype(jnp.float32)
        mixed = jnp.einsum('hqk,khd->qhd', rounded, value_heads)
        square_mean = lax.optimization_barrier(jnp.mean(mixed * mixed, axis=-1, keepdims=True))
        return (mixed * lax.rsqrt(square_mean + head_eps) * head_gain).astype(jnp.bfloat16)
    begins = jnp.arange(SEQUENCE_TOKENS // block_rows, dtype=jnp.int32) * block_rows
    att_out = lax.map(one_block, begins).reshape(SEQUENCE_TOKENS, SB_WIDTH)
    mixer = jnp.dot(att_out, out_weight, preferred_element_type=jnp.float32)
    hidden_in = layer_norm(residual_scale * residual.astype(jnp.float32) + mixer, ln1_gain, ln1_bias).astype(jnp.bfloat16)
    flat_ids = expert_ids.reshape(-1)
    limit = N_SP * N_TP * CAP
    hidden_units = FF // N_TP

    def per_expert(collected, expert):
        found = jnp.nonzero(flat_ids == expert, size=limit, fill_value=SEQUENCE_TOKENS * TOP)[0].astype(jnp.int32)
        token_rows = hidden_in[jnp.minimum(found // TOP, SEQUENCE_TOKENS - 1)]
        gate_part = jnp.dot(token_rows, gate_weight[expert], preferred_element_type=jnp.float32)
        up_part = jnp.dot(token_rows, up_weight[expert], preferred_element_type=jnp.float32)
        active = (jax.nn.silu(gate_part) * up_part).astype(jnp.bfloat16)
        summed = jnp.zeros((limit, D), jnp.float32)
        for index in range(N_TP):
            part = jnp.dot(active[:, index * hidden_units:(index + 1) * hidden_units], down_weight[expert, index * hidden_units:(index + 1) * hidden_units], preferred_element_type=jnp.float32)
            summed = summed + lax.optimization_barrier(part.astype(jnp.bfloat16)).astype(jnp.float32)
        collected = collected.at[found].set(summed.astype(jnp.bfloat16), mode='drop')
        return (collected, None)
    collected, _ = lax.scan(per_expert, jnp.zeros((SEQUENCE_TOKENS * TOP, D), jnp.bfloat16), jnp.arange(EXPERTS, dtype=jnp.int32))
    gates = jax.nn.softmax(route_logits.astype(jnp.float32), axis=-1)
    routed = lax.optimization_barrier(jnp.sum(gates[:, :, None] * collected.reshape(SEQUENCE_TOKENS, TOP, D).astype(jnp.float32), axis=1))
    return layer_norm(residual_scale * hidden_in.astype(jnp.float32) + routed, ln2_gain, ln2_bias).astype(jnp.bfloat16)
```

```python
import jax
import jax.numpy as jnp
from jax import lax
from jax.experimental import pallas as pl
from jax.experimental.pallas import tpu as pltpu
from jax.sharding import Mesh
from jax.sharding import PartitionSpec as P

residual_scale = 8.0**0.25
norm_eps = 1e-05
head_eps = 1e-06


f32 = jnp.float32
bf16 = jnp.bfloat16
SUB = 8
LANES = 128
EXTRA = 16


def nt_dot(a, b):
    return lax.dot_general(a, b, (((1,), (1,)), ((), ())), preferred_element_type=f32)


def shift(x, axis, step, size, wrap=True):
    pairs = [(i, (i + step) % size) for i in range(size) if wrap or 0 <= i + step < size]
    return lax.ppermute(x, axis, pairs)


def vmem_call(body, out_shape, scratch=(), smem=0, operands=0, **kw):
    specs = [pl.BlockSpec(memory_space=pltpu.SMEM)] * smem
    specs += [pl.BlockSpec(memory_space=pltpu.VMEM)] * (operands - smem)
    return pl.pallas_call(
        body,
        out_shape=out_shape,
        in_specs=specs,
        out_specs=jax.tree.map(lambda _: pl.BlockSpec(memory_space=pltpu.VMEM), out_shape),
        scratch_shapes=list(scratch),
        compiler_params=pltpu.CompilerParams(vmem_limit_bytes=56 * 1024 * 1024),
        **kw,
    )


def pack_body(k_ref, v_ref, out_ref):
    rows = k_ref.shape[0]
    heads = k_ref.shape[1] // LANES
    per = rows // SUB
    r = lax.broadcasted_iota(jnp.int32, (rows, rows), 0)
    s = lax.broadcasted_iota(jnp.int32, (rows, rows), 1)
    pick = ((r % SUB) * per + r // SUB == s).astype(f32).astype(bf16)
    ks = jnp.dot(pick, k_ref[...], preferred_element_type=f32).astype(bf16)
    vs = jnp.dot(pick, v_ref[...], preferred_element_type=f32)
    for h in range(heads):
        out_ref[h, 0:rows, :] = ks[:, h * LANES : (h + 1) * LANES]
        for p in range(rows // LANES):
            part = vs[p * LANES : (p + 1) * LANES, h * LANES : (h + 1) * LANES]
            out_ref[h, rows + p * LANES : rows + (p + 1) * LANES, :] = part.T.astype(bf16)


def attend_body(nz, nx, nc, off_ref, meta_ref, *refs):
    q_refs, refs = refs[:nz], refs[nz:]
    own_refs, refs = refs[:nx], refs[nx:]
    twin_refs, refs = refs[:nx], refs[nx:]
    p_refs, (kv, qs, ps, acc, surv) = refs[:nz], refs[nz:]
    z, x, c = meta_ref[0], meta_ref[1], meta_ref[2]
    own_block = x * nc + c
    blocks = nx * nc
    rows = qs.shape[2]
    heads = qs.shape[1]
    scale = LANES ** (-0.5)
    for r in range(nx):
        at = (x + (nx - r)) % nx
        kv[at * nc + c] = own_refs[r][...]
        kv[at * nc + (1 - c)] = twin_refs[r][...]
    for s in range(nz):
        for h in range(heads):
            qs[s, h] = q_refs[s][:, h * LANES : (h + 1) * LANES]
    sub = lax.broadcasted_iota(jnp.int32, (SUB, LANES), 0)
    lane = lax.broadcasted_iota(jnp.int32, (SUB, LANES), 1)
    per = rows // SUB

    def tile(j, s, h, offset, masked):
        scores = nt_dot(kv[j, h, 0:rows, :], qs[s, h])
        columns = []
        for p in range(rows // LANES):
            part = scores[:, p * LANES : (p + 1) * LANES]
            run = jnp.zeros((SUB, LANES), f32)
            logs = [None] * per
            for i in reversed(range(per)):
                v = part[i * SUB : (i + 1) * SUB] * scale - offset
                drop = jnp.maximum(v, jnp.log(1.0 + jnp.exp(jnp.minimum(v, 60.0))))
                if masked:
                    seen = sub * per + i < lane + p * LANES
                    drop = jnp.where(seen, drop, 0.0)
                run = run + drop
                logs[i] = v - run
                if masked:
                    logs[i] = jnp.where(seen, logs[i], -1e30)
            tail = run
            for d in (1, 2, 4):
                tail = tail + jnp.where(sub < SUB - d, pltpu.roll(tail, SUB - d, 0), 0.0)
            before = surv[:, p * LANES : (p + 1) * LANES]
            base = before + jnp.where(sub < SUB - 1, pltpu.roll(tail, SUB - 1, 0), 0.0)
            weights = jnp.concatenate([jnp.exp(u - base) for u in logs], axis=0)
            columns.append(weights.astype(bf16))
            surv[:, p * LANES : (p + 1) * LANES] = before + jnp.broadcast_to(
                tail[0:1], (SUB, LANES)
            )
        weights = jnp.concatenate(columns, axis=1)
        vt = jnp.concatenate(
            [
                kv[j, h, rows + p * LANES : rows + (p + 1) * LANES, :]
                for p in range(rows // LANES)
            ],
            axis=1,
        )
        acc[...] += jnp.dot(vt, weights, preferred_element_type=f32)

    def one(t, _):
        s = t // heads
        h = t % heads
        offset = off_ref[h]
        acc[...] = jnp.zeros_like(acc)
        surv[...] = jnp.zeros_like(surv)

        @pl.when(s == 0)
        def _():
            tile(own_block, s, h, offset, True)

        count = jnp.where(s == 0, own_block, blocks)

        def turn(k, _):
            tile(count - 1 - k, s, h, offset, False)
            return 0

        lax.fori_loop(0, count, turn, 0)
        ps[s, h, 0:LANES, :] = acc[...].astype(bf16)
        total = surv[...]
        high = total.astype(bf16).astype(f32)
        mid = (total - high).astype(bf16).astype(f32)
        low = total - high - mid
        wide = lax.broadcasted_iota(jnp.int32, total.shape, 0)
        split = jnp.where(wide == 0, high, jnp.where(wide == 1, mid, jnp.where(wide == 2, low, 0.0)))
        ps[s, h, LANES : LANES + EXTRA, :] = jnp.concatenate(
            [split, jnp.zeros_like(split)], axis=0
        ).astype(bf16)
        return 0

    lax.fori_loop(0, (nz - z) * heads, one, 0)
    for s in range(nz):

        @pl.when(s < nz - z)
        def _():
            p_refs[s][...] = ps[s]

        @pl.when(s >= nz - z)
        def _():
            p_refs[s][...] = jnp.zeros_like(p_refs[s])


def join_body(nz, ntp, meta_ref, *refs):
    p_refs, gain_ref, refs = refs[:nz], refs[nz], refs[nz + 1 :]
    out_refs, (whole,) = refs[:ntp], refs[ntp:]
    y = meta_ref[3]
    heads, _, rows = p_refs[0].shape
    for h in range(heads):
        total = jnp.zeros((LANES, rows), f32)
        gone = jnp.zeros((1, rows), f32)
        for s in range(nz):
            total = total + p_refs[s][h, 0:LANES, :].astype(f32) * jnp.exp(-gone)
            split = p_refs[s][h, LANES : LANES + EXTRA, :].astype(f32)
            gone = gone + jnp.sum(split, axis=0, keepdims=True)
        square = jnp.mean(total * total, axis=0, keepdims=True)
        normed = total * lax.rsqrt(square + head_eps) * gain_ref[...]
        whole[:, h * LANES : (h + 1) * LANES] = normed.T
    count = rows // ntp
    for s in range(ntp):
        at = pl.multiple_of(((y + s) % ntp) * count, count)
        out_refs[s][...] = whole[pl.ds(at, count), :].astype(bf16)


def norm_rows(value, gain, bias):
    mean = jnp.mean(value, axis=-1, keepdims=True)
    centred = value - mean
    variance = jnp.mean(centred * centred, axis=-1, keepdims=True)
    return centred * lax.rsqrt(variance + norm_eps) * gain + bias


def mix_body(a0, a1, a2, a3, w0, w1, w2a, w2b, w3, res_ref, gain_ref, bias_ref, out_ref):
    half = w2a.shape[0]
    dot = lambda a, w: jnp.dot(a, w[...], preferred_element_type=f32)
    mixed = dot(a0[...], w0) + dot(a1[...], w1) + dot(a3[...], w3)
    mixed = mixed + dot(a2[:, :half], w2a) + dot(a2[:, half:], w2b)
    value = residual_scale * res_ref[...].astype(f32) + mixed
    out_ref[...] = norm_rows(value, gain_ref[...], bias_ref[...]).astype(bf16)


def spread4(x, axis):
    half = x.shape[0] // 2
    left = shift(x, axis, 1, 4)
    right = shift(x, axis, -1, 4)
    far_top = shift(left[:half], axis, 1, 4)
    far_bottom = shift(right[half:], axis, -1, 4)
    return x, left, far_top, far_bottom, right


def mixer(queries, keys, values, score_offset, head_gain, out_weight, residual, gain, bias):
    nz, nx, nc, ntp = (lax.axis_size(a) for a in ("z", "x", "c", "tp"))
    rows = queries.shape[0]
    heads = queries.shape[1] // LANES
    sds = jax.ShapeDtypeStruct
    slot = lax.broadcasted_iota(jnp.int32, (4,), 0)
    meta = jnp.where(
        slot == 0,
        lax.axis_index("z"),
        jnp.where(
            slot == 1,
            lax.axis_index("x"),
            jnp.where(slot == 2, lax.axis_index("c"), lax.axis_index("tp")),
        ),
    )
    packed = vmem_call(
        pack_body, sds((heads, 2 * rows, LANES), bf16), operands=2, name="pack"
    )(keys, values)
    own = [packed] + [shift(packed, "x", s, nx) for s in range(1, nx)]
    twin = [shift(o, "c", 1, nc) for o in own]
    asked = [queries] + [shift(queries, "z", -s, nz, wrap=False) for s in range(1, nz)]
    weights = spread4(out_weight, "tp")
    partial = sds((heads, LANES + EXTRA, rows), bf16)
    parts = vmem_call(
        lambda *r: attend_body(nz, nx, nc, *r),
        [partial] * nz,
        scratch=[
            pltpu.VMEM((nx * nc, heads, 2 * rows, LANES), bf16),
            pltpu.VMEM((nz, heads, rows, LANES), bf16),
            pltpu.VMEM((nz, heads, LANES + EXTRA, rows), bf16),
            pltpu.VMEM((LANES, rows), f32),
            pltpu.VMEM((SUB, rows), f32),
        ],
        smem=2,
        operands=2 + nz + 2 * nx,
        name="attend",
    )(score_offset, meta, *asked, *own, *twin)
    back = [parts[0]] + [shift(parts[s], "z", s, nz, wrap=False) for s in range(1, nz)]
    pieces = vmem_call(
        lambda *r: join_body(nz, ntp, *r),
        [sds((rows // ntp, heads * LANES), bf16)] * ntp,
        scratch=[pltpu.VMEM((rows, heads * LANES), f32)],
        smem=1,
        operands=2 + nz,
        name="join",
    )(meta, *back, head_gain[:, None])
    got = [pieces[0]] + [shift(pieces[s], "tp", s, ntp) for s in range(1, ntp)]
    return vmem_call(mix_body, sds(residual.shape, bf16), operands=12, name="mix")(
        *got, *weights, residual, gain[None], bias[None]
    )


SP = ("z", "x", "c")


def split_up(x, dim, size):
    dims = x.shape
    parts = x.reshape(*dims[:dim], size, dims[dim] // size, *dims[dim + 1 :])
    return jnp.moveaxis(parts, dim, 0)


def summed_on_arrival(x, axis, dim):
    size = lax.axis_size(axis)
    parts = lax.all_to_all(split_up(x, dim, size), axis, 0, 0, tiled=True)
    return jnp.sum(parts.astype(jnp.float32), axis=0)


def layer_norm(inputs, gain, shift):
    mean_value = jnp.mean(inputs, axis=-1, keepdims=True)
    centred = inputs - mean_value
    variance = jnp.mean(centred * centred, axis=-1, keepdims=True)
    return centred * lax.rsqrt(variance + norm_eps) * gain + shift


def on_device(
    queries,
    keys,
    values,
    score_offset,
    head_gain,
    out_weight,
    residual,
    ln1_gain,
    ln1_bias,
    expert_ids,
    route_logits,
    gate_weight,
    up_weight,
    down_weight,
    ln2_gain,
    ln2_bias,
):
    row_count = residual.shape[0]
    model_width = residual.shape[1]
    hidden_in = mixer(
        queries, keys, values, score_offset, head_gain, out_weight, residual, ln1_gain, ln1_bias
    )
    top_count = expert_ids.shape[1]
    experts = lax.axis_size(SP)
    capacity = max(2, 2 * top_count * row_count // experts)
    flat_ids = expert_ids.reshape(-1)
    onehot = (flat_ids[:, None] == jnp.arange(experts, dtype=jnp.int32)[None, :]).astype(jnp.int32)
    slot_index = jnp.sum(jnp.cumsum(onehot, axis=0) * onehot, axis=1) - 1
    destination = flat_ids * capacity + slot_index
    send_rows = jnp.repeat(hidden_in, top_count, axis=0)
    outgoing = (
        jnp.zeros((experts * capacity, model_width), jnp.bfloat16).at[destination].set(send_rows)
    )
    outgoing = outgoing.reshape(experts, capacity, model_width)
    row_block = lax.all_gather(
        lax.all_to_all(outgoing, SP, split_axis=0, concat_axis=0, tiled=True),
        "tp",
        axis=0,
        tiled=True,
    )
    block_count = row_block.shape[0]
    flat_rows = row_block.reshape(-1, model_width)
    gate_part = jnp.dot(flat_rows, gate_weight[0], preferred_element_type=jnp.float32)
    up_part = jnp.dot(flat_rows, up_weight[0], preferred_element_type=jnp.float32)
    active = (jax.nn.silu(gate_part) * up_part).astype(jnp.bfloat16)
    down_part = jnp.dot(active, down_weight[0], preferred_element_type=jnp.float32).astype(
        jnp.bfloat16
    )
    partials = down_part.reshape(block_count, -1, model_width)
    summed = summed_on_arrival(partials, "tp", 0).astype(jnp.bfloat16)
    returned_rows = lax.all_to_all(summed, SP, split_axis=0, concat_axis=0, tiled=True)
    picked = returned_rows.reshape(experts * capacity, model_width)[destination].reshape(
        row_count, top_count, model_width
    )
    gates = jax.nn.softmax(route_logits, axis=-1)
    routed = jnp.sum(gates[:, :, None] * picked.astype(jnp.float32), axis=1)
    return layer_norm(
        residual_scale * hidden_in.astype(jnp.float32) + routed, ln2_gain, ln2_bias
    ).astype(jnp.bfloat16)


def solution(mesh):
    nz, nx, nc = 8, 4, 2
    mesh = Mesh(mesh.devices.reshape(nz, nx, nc, mesh.shape["tp"]), ("z", "x", "c", "tp"))
    in_specs = (
        P(SP, "tp"),
        P(SP, "tp"),
        P(SP, "tp"),
        P("tp"),
        P(),
        P("tp", None),
        P((*SP, "tp"), None),
        P(),
        P(),
        P((*SP, "tp"), None),
        P((*SP, "tp"), None),
        P(SP, None, "tp"),
        P(SP, None, "tp"),
        P(SP, "tp", None),
        P(),
        P(),
    )
    out_specs = P((*SP, "tp"), None)
    return jax.shard_map(
        on_device, mesh=mesh, in_specs=in_specs, out_specs=out_specs, check_vma=False
    )
```

```python
import jax
import jax.numpy as jnp
from jax import lax
from jax.experimental import pallas as pl
from jax.experimental.pallas import tpu as pltpu
from jax.sharding import Mesh
from jax.sharding import PartitionSpec as P

residual_scale = 8.0**0.25
norm_eps = 1e-05
head_eps = 1e-06


f32 = jnp.float32
bf16 = jnp.bfloat16
SUB = 8
LANES = 128
SPOT = 16
EXTRA = 16


def nt_dot(a, b):
    return lax.dot_general(a, b, (((1,), (1,)), ((), ())), preferred_element_type=f32)


def shift(x, axis, step, size, wrap=True):
    pairs = [(i, (i + step) % size) for i in range(size) if wrap or 0 <= i + step < size]
    return lax.ppermute(x, axis, pairs)


def vmem_call(body, out_shape, scratch=(), smem=0, operands=0, **kw):
    specs = [pl.BlockSpec(memory_space=pltpu.SMEM)] * smem
    specs += [pl.BlockSpec(memory_space=pltpu.VMEM)] * (operands - smem)
    return pl.pallas_call(
        body,
        out_shape=out_shape,
        in_specs=specs,
        out_specs=jax.tree.map(lambda _: pl.BlockSpec(memory_space=pltpu.VMEM), out_shape),
        scratch_shapes=list(scratch),
        compiler_params=pltpu.CompilerParams(vmem_limit_bytes=56 * 1024 * 1024),
        **kw,
    )


def pack_body(k_ref, v_ref, out_ref):
    rows = k_ref.shape[0]
    heads = k_ref.shape[1] // LANES
    per = rows // SUB
    r = lax.broadcasted_iota(jnp.int32, (rows, rows), 0)
    s = lax.broadcasted_iota(jnp.int32, (rows, rows), 1)
    pick = ((r % SUB) * per + r // SUB == s).astype(f32).astype(bf16)
    ks = jnp.dot(pick, k_ref[...], preferred_element_type=f32).astype(bf16)
    vs = jnp.dot(pick, v_ref[...], preferred_element_type=f32)
    for h in range(heads):
        out_ref[h, 0:rows, :] = ks[:, h * LANES : (h + 1) * LANES]
        for p in range(rows // LANES):
            part = vs[p * LANES : (p + 1) * LANES, h * LANES : (h + 1) * LANES]
            out_ref[h, rows + p * LANES : rows + (p + 1) * LANES, :] = part.T.astype(bf16)


def attend_body(nz, nx, nc, off_ref, meta_ref, *refs):
    q_refs, refs = refs[:nz], refs[nz:]
    own_refs, refs = refs[:nx], refs[nx:]
    twin_refs, refs = refs[:nx], refs[nx:]
    p_refs, (kv, qs, ps, acc, surv, first, second, late) = refs[:nz], refs[nz:]
    z, x, c = meta_ref[0], meta_ref[1], meta_ref[2]
    own_block = x * nc + c
    blocks = nx * nc
    rows = qs.shape[2]
    heads = qs.shape[1]
    scale = LANES ** (-0.5)
    for r in range(nx):
        at = (x + (nx - r)) % nx
        kv[at * nc + c] = own_refs[r][...]
        kv[at * nc + (1 - c)] = twin_refs[r][...]
    for s in range(nz):
        for h in range(heads):
            qs[s, h] = q_refs[s][:, h * LANES : (h + 1) * LANES]
    sub = lax.broadcasted_iota(jnp.int32, (SUB, LANES), 0)
    lane = lax.broadcasted_iota(jnp.int32, (SUB, LANES), 1)
    per = rows // SUB

    def score(j, s, h):
        return nt_dot(kv[j, h, 0:rows, :], qs[s, h])

    def weigh(scores, h, masked):
        offset = off_ref[h]
        columns = []
        for p in range(rows // LANES):
            run = jnp.zeros((SUB, LANES), f32)
            logs = [None] * per
            for i in reversed(range(per)):
                part = scores[i * SUB : (i + 1) * SUB, p * LANES : (p + 1) * LANES]
                v = part * scale - offset
                drop = jnp.maximum(v, jnp.log(1.0 + jnp.exp(jnp.minimum(v, 60.0))))
                if masked:
                    seen = sub * per + i < lane + p * LANES
                    drop = jnp.where(seen, drop, 0.0)
                run = run + drop
                logs[i] = v - run
                if masked:
                    logs[i] = jnp.where(seen, logs[i], -1e30)
            tail = run
            for d in (1, 2, 4):
                tail = tail + jnp.where(sub < SUB - d, pltpu.roll(tail, SUB - d, 0), 0.0)
            before = surv[h, :, p * LANES : (p + 1) * LANES]
            base = before + jnp.where(sub < SUB - 1, pltpu.roll(tail, SUB - 1, 0), 0.0)
            weights = jnp.concatenate([jnp.exp(u - base) for u in logs], axis=0)
            columns.append(weights.astype(bf16))
            surv[h, :, p * LANES : (p + 1) * LANES] = before + jnp.broadcast_to(
                tail[0:1], (SUB, LANES)
            )
        return jnp.concatenate(columns, axis=1)

    def add_values(j, h, weights):
        vt = jnp.concatenate(
            [
                kv[j, h, rows + p * LANES : rows + (p + 1) * LANES, :]
                for p in range(rows // LANES)
            ],
            axis=1,
        )
        acc[h] += jnp.dot(vt, weights, preferred_element_type=f32)

    def one(s, _):
        acc[...] = jnp.zeros_like(acc)
        surv[...] = jnp.zeros_like(surv)
        late[...] = jnp.zeros_like(late)

        @pl.when(s == 0)
        def _():
            for h in range(heads):
                add_values(own_block, h, weigh(score(own_block, s, h), h, True))

        count = jnp.where(s == 0, own_block, blocks)
        first[...] = score(jnp.maximum(count - 1, 0), s, 0)

        def turn(k, _):
            j = count - 1 - k
            second[...] = score(j, s, 1)
            add_values(jnp.minimum(j + 1, blocks - 1), 1, late[...])
            weights = weigh(first, 0, False)
            first[...] = score(jnp.maximum(j - 1, 0), s, 0)
            add_values(j, 0, weights)
            late[...] = weigh(second, 1, False)
            return 0

        lax.fori_loop(0, count, turn, 0)
        add_values(0, 1, late[...])
        for h in range(heads):
            ps[s, h, 0:LANES, :] = acc[h].astype(bf16)
            total = surv[h]
            high = total.astype(bf16).astype(f32)
            mid = (total - high).astype(bf16).astype(f32)
            low = total - high - mid
            wide = lax.broadcasted_iota(jnp.int32, total.shape, 0)
            split = jnp.where(
                wide == 0, high, jnp.where(wide == 1, mid, jnp.where(wide == 2, low, 0.0))
            )
            ps[s, h, LANES : LANES + EXTRA, :] = jnp.concatenate(
                [split, jnp.zeros_like(split)], axis=0
            ).astype(bf16)
        return 0

    lax.fori_loop(0, nz - z, one, 0)
    for s in range(nz):

        @pl.when(s < nz - z)
        def _():
            p_refs[s][...] = ps[s]

        @pl.when(s >= nz - z)
        def _():
            p_refs[s][...] = jnp.zeros_like(p_refs[s])


def join_body(nz, ntp, meta_ref, *refs):
    p_refs, gain_ref, refs = refs[:nz], refs[nz], refs[nz + 1 :]
    out_refs, (whole,) = refs[:ntp], refs[ntp:]
    y = meta_ref[3]
    heads, _, rows = p_refs[0].shape
    for h in range(heads):
        total = jnp.zeros((LANES, rows), f32)
        gone = jnp.zeros((1, rows), f32)
        for s in range(nz):
            total = total + p_refs[s][h, 0:LANES, :].astype(f32) * jnp.exp(-gone)
            split = p_refs[s][h, LANES : LANES + EXTRA, :].astype(f32)
            gone = gone + jnp.sum(split, axis=0, keepdims=True)
        square = jnp.mean(total * total, axis=0, keepdims=True)
        normed = total * lax.rsqrt(square + head_eps) * gain_ref[...]
        whole[:, h * LANES : (h + 1) * LANES] = normed.T
    count = rows // ntp
    for s in range(ntp):
        at = pl.multiple_of(((y + s) % ntp) * count, count)
        out_refs[s][...] = whole[pl.ds(at, count), :].astype(bf16)


def norm_rows(value, gain, bias):
    mean = jnp.mean(value, axis=-1, keepdims=True)
    centred = value - mean
    variance = jnp.mean(centred * centred, axis=-1, keepdims=True)
    return centred * lax.rsqrt(variance + norm_eps) * gain + bias


def mix_body(chunks, a0, a1, a2, a3, w0, w1, w2a, w2b, w3, res_ref, gain_ref, bias_ref, *refs):
    target_refs, (hidden_ref, *send_refs) = refs[:chunks], refs[chunks:]
    half = w2a.shape[0]
    dot = lambda a, w: jnp.dot(a, w[...], preferred_element_type=f32)
    mixed = dot(a0[...], w0) + dot(a1[...], w1) + dot(a3[...], w3)
    mixed = mixed + dot(a2[:, :half], w2a) + dot(a2[:, half:], w2b)
    value = residual_scale * res_ref[...].astype(f32) + mixed
    hidden = norm_rows(value, gain_ref[...], bias_ref[...]).astype(bf16)
    hidden_ref[...] = hidden
    for target, send in zip(target_refs, send_refs):
        count, width = send.shape
        folds = hidden.shape[1] // width
        stack = jnp.concatenate(
            [hidden[:, q * width : (q + 1) * width] for q in range(folds)], axis=0
        )
        row = lax.broadcasted_iota(jnp.int32, (count, stack.shape[0]), 0)
        pick = (row == target[0:1, :]) | (row == target[1:2, :])
        pick = jnp.where(pick, 1.0, 0.0).astype(bf16)
        send[...] = jnp.dot(pick, stack, preferred_element_type=f32).astype(bf16)


def fold_order(size, slots, turned):
    folds = SPOT // slots
    sources = size // SPOT
    axis = 1 if turned else 0
    to = lax.broadcasted_iota(jnp.int32, (size, size), axis)
    at = lax.broadcasted_iota(jnp.int32, (size, size), 1 - axis)
    q, rest = to // (sources * slots), to % (sources * slots)
    want = (rest // slots) * SPOT + q * slots + rest % slots
    return jnp.where(want == at, 1.0, 0.0).astype(bf16)


def expert_body(slots, own, left, far_top, far_bottom, right, wg_any, wu_any, wd_any, *refs):
    outs, (x, y, wg, wu, wd, sems) = refs[:7], refs[7:]
    loads = [
        pltpu.make_async_copy(src.at[0], dst, sems.at[i])
        for i, (src, dst) in enumerate(((wg_any, wg), (wu_any, wu), (wd_any, wd)))
    ]
    for load in loads:
        load.start()
    width = own.shape[1]
    folds = SPOT // slots
    group = 16 * SPOT
    kept = 16 * slots
    to_folds = fold_order(group, slots, False)
    base = 0
    for piece in (own, left, right, far_top, far_bottom):
        for g in range(piece.shape[0] // group):
            rows = jnp.dot(
                to_folds, piece[g * group : (g + 1) * group], preferred_element_type=f32
            ).astype(bf16)
            for q in range(folds):
                x[base : base + kept, q * width : (q + 1) * width] = rows[
                    q * kept : (q + 1) * kept
                ]
            base += kept
    loads[0].wait()
    loads[1].wait()
    loads[2].wait()
    step = min(512, x.shape[0])
    hidden = wg.shape[1]
    part = 256

    def turn(m, _):
        at = pl.multiple_of(m * step, step)
        rows = x[pl.ds(at, step), :]
        active = []
        for n in range(0, hidden, part):
            gate = jnp.dot(rows, wg[:, n : n + part], preferred_element_type=f32)
            up = jnp.dot(rows, wu[:, n : n + part], preferred_element_type=f32)
            active.append((gate / (1.0 + jnp.exp(-gate)) * up).astype(bf16))
        active = jnp.concatenate(active, axis=1)
        for n in range(0, x.shape[1], part):
            y[pl.ds(at, step), n : n + part] = jnp.dot(
                active, wd[:, n : n + part], preferred_element_type=f32
            ).astype(bf16)
        return 0

    lax.fori_loop(0, x.shape[0] // step, turn, 0)
    from_folds = fold_order(group, slots, True)
    base = 0
    for out in outs:
        for g in range(out.shape[0] // group):
            rows = jnp.concatenate(
                [y[base : base + kept, q * width : (q + 1) * width] for q in range(folds)], axis=0
            )
            out[g * group : (g + 1) * group] = jnp.dot(
                from_folds, rows, preferred_element_type=f32
            ).astype(bf16)
            base += kept


def total_body(own, r1a, r1b, r2a, r2b, out):
    half = r1a.shape[0]
    for i, (a, b) in enumerate(((r1a, r2a), (r1b, r2b))):
        rows = slice(i * half, (i + 1) * half)
        out[rows] = (own[rows].astype(f32) + a[...].astype(f32) + b[...].astype(f32)).astype(bf16)


def finish_body(chunks, logits_ref, hidden_ref, gain_ref, bias_ref, *refs):
    target_refs, back_refs, (out_ref,) = refs[:chunks], refs[chunks : 2 * chunks], refs[2 * chunks :]
    logits = logits_ref[...]
    top = jnp.max(logits, axis=1, keepdims=True)
    raised = jnp.exp(logits - top)
    gates = raised / jnp.sum(raised, axis=1, keepdims=True)
    count, model = hidden_ref.shape
    choices = logits.shape[1]
    routed = None
    for target, back in zip(target_refs, back_refs):
        width = back.shape[1]
        folds = model // width
        at = lax.broadcasted_iota(jnp.int32, (target.shape[0], back.shape[0]), 1)
        pick = jnp.where(at == target[...], 1.0, 0.0).astype(bf16)
        rows = jnp.dot(pick, back[...], preferred_element_type=f32)
        mine = None
        for k in range(choices):
            spread = jnp.concatenate(
                [rows[(k * folds + q) * count : (k * folds + q + 1) * count] for q in range(folds)],
                axis=1,
            )
            spread = gates[:, k : k + 1] * spread
            mine = spread if mine is None else mine + spread
        routed = mine if routed is None else routed + mine
    value = residual_scale * hidden_ref[...].astype(f32) + routed
    out_ref[...] = norm_rows(value, gain_ref[...], bias_ref[...]).astype(bf16)


def targets(expert_ids, capacity, chunks):
    count, choices = expert_ids.shape
    flat = expert_ids.T.reshape(-1)
    earlier = jnp.arange(flat.shape[0])[:, None] > jnp.arange(flat.shape[0])[None, :]
    same = flat[:, None] == flat[None, :]
    slot = jnp.sum((same & earlier).astype(jnp.int32), axis=1)
    slots = capacity // chunks
    folds = SPOT // slots
    fold = jnp.arange(folds, dtype=jnp.int32)[None, :, None]
    base = (flat * SPOT + slot % slots).reshape(choices, 1, count) + fold * slots
    part = (slot // slots).reshape(choices, 1, count)
    return [jnp.where(part == c, base, -1) for c in range(chunks)]


def spread4(x, axis):
    half = x.shape[0] // 2
    left = shift(x, axis, 1, 4)
    right = shift(x, axis, -1, 4)
    far_top = shift(left[:half], axis, 1, 4)
    far_bottom = shift(right[half:], axis, -1, 4)
    return x, left, far_top, far_bottom, right


def mixer(
    queries, keys, values, score_offset, head_gain, out_weight, residual, gain, bias, aims, experts
):
    nz, nx, nc, ntp = (lax.axis_size(a) for a in ("z", "x", "c", "tp"))
    rows = queries.shape[0]
    heads = queries.shape[1] // LANES
    sds = jax.ShapeDtypeStruct
    slot = lax.broadcasted_iota(jnp.int32, (4,), 0)
    meta = jnp.where(
        slot == 0,
        lax.axis_index("z"),
        jnp.where(
            slot == 1,
            lax.axis_index("x"),
            jnp.where(slot == 2, lax.axis_index("c"), lax.axis_index("tp")),
        ),
    )
    packed = vmem_call(
        pack_body, sds((heads, 2 * rows, LANES), bf16), operands=2, name="pack"
    )(keys, values)
    own = [packed] + [shift(packed, "x", s, nx) for s in range(1, nx)]
    twin = [shift(o, "c", 1, nc) for o in own]
    asked = [queries] + [shift(queries, "z", -s, nz, wrap=False) for s in range(1, nz)]
    weights = spread4(out_weight, "tp")
    partial = sds((heads, LANES + EXTRA, rows), bf16)
    parts = vmem_call(
        lambda *r: attend_body(nz, nx, nc, *r),
        [partial] * nz,
        scratch=[
            pltpu.VMEM((nx * nc, heads, 2 * rows, LANES), bf16),
            pltpu.VMEM((nz, heads, rows, LANES), bf16),
            pltpu.VMEM((nz, heads, LANES + EXTRA, rows), bf16),
            pltpu.VMEM((heads, LANES, rows), f32),
            pltpu.VMEM((heads, SUB, rows), f32),
            pltpu.VMEM((rows, rows), f32),
            pltpu.VMEM((rows, rows), f32),
            pltpu.VMEM((rows, rows), bf16),
        ],
        smem=2,
        operands=2 + nz + 2 * nx,
        name="attend",
    )(score_offset, meta, *asked, *own, *twin)
    back = [parts[0]] + [shift(parts[s], "z", s, nz, wrap=False) for s in range(1, nz)]
    pieces = vmem_call(
        lambda *r: join_body(nz, ntp, *r),
        [sds((rows // ntp, heads * LANES), bf16)] * ntp,
        scratch=[pltpu.VMEM((rows, heads * LANES), f32)],
        smem=1,
        operands=2 + nz,
        name="join",
    )(meta, *back, head_gain[:, None])
    got = [pieces[0]] + [shift(pieces[s], "tp", s, ntp) for s in range(1, ntp)]
    chunks = len(aims)
    folds = aims[0].shape[1]
    width = residual.shape[1] // folds
    return vmem_call(
        lambda *r: mix_body(chunks, *r),
        [sds(residual.shape, bf16)] + [sds((experts * SPOT, width), bf16)] * chunks,
        operands=12 + chunks,
        name="mix",
    )(*got, *weights, residual, gain[None], bias[None], *[a.reshape(a.shape[0], -1) for a in aims])


def run_experts(pieces, gate_weight, up_weight, down_weight, slots):
    own = pieces[0]
    half = pieces[2]
    sds = jax.ShapeDtypeStruct
    total = sum(p.shape[0] for p in pieces) * slots // SPOT
    model, hidden = gate_weight.shape[1:]
    outs = [sds(own.shape, bf16)] + [sds(half.shape, bf16)] * 6
    vmem = pl.BlockSpec(memory_space=pltpu.VMEM)
    return pl.pallas_call(
        lambda *r: expert_body(slots, *r),
        out_shape=outs,
        in_specs=[vmem] * 5 + [pl.BlockSpec(memory_space=pl.ANY)] * 3,
        out_specs=[vmem] * 7,
        scratch_shapes=[
            pltpu.VMEM((total, model), bf16),
            pltpu.VMEM((total, model), bf16),
            pltpu.VMEM((model, hidden), bf16),
            pltpu.VMEM((model, hidden), bf16),
            pltpu.VMEM((hidden, model), bf16),
            pltpu.SemaphoreType.DMA((3,)),
        ],
        compiler_params=pltpu.CompilerParams(vmem_limit_bytes=56 * 1024 * 1024),
        name="experts",
    )(*pieces, gate_weight, up_weight, down_weight)


def add_up(parts):
    own, left_top, left_bottom, right_top, right_bottom, far_top, far_bottom = parts
    add = lambda a, b: (a.astype(f32) + b.astype(f32)).astype(bf16)
    from_left = shift(far_top, "tp", 1, 4)
    from_right = shift(far_bottom, "tp", -1, 4)
    r1b = shift(right_bottom, "tp", 1, 4)
    r2a = shift(left_top, "tp", -1, 4)
    r1a = shift(add(right_top, from_left), "tp", 1, 4)
    r2b = shift(add(left_bottom, from_right), "tp", -1, 4)
    return vmem_call(
        total_body, jax.ShapeDtypeStruct(own.shape, bf16), operands=5, name="total"
    )(own, r1a, r1b, r2a, r2b)


def exchange(rows):
    parts = rows.reshape(-1, SPOT, rows.shape[1])
    return lax.all_to_all(parts, SP, 0, 0, tiled=True).reshape(rows.shape)


SP = ("z", "x", "c")
CHUNKS = 1


def on_device(
    queries,
    keys,
    values,
    score_offset,
    head_gain,
    out_weight,
    residual,
    ln1_gain,
    ln1_bias,
    expert_ids,
    route_logits,
    gate_weight,
    up_weight,
    down_weight,
    ln2_gain,
    ln2_bias,
):
    row_count = residual.shape[0]
    top_count = expert_ids.shape[1]
    experts = lax.axis_size(SP)
    capacity = max(2, 2 * top_count * row_count // experts)
    chunks = CHUNKS
    slots = capacity // chunks
    aims = targets(expert_ids, capacity, chunks)
    hidden_in, *outgoing = mixer(
        queries,
        keys,
        values,
        score_offset,
        head_gain,
        out_weight,
        residual,
        ln1_gain,
        ln1_bias,
        aims,
        experts,
    )
    returned = []
    for rows in outgoing:
        pieces = spread4(exchange(rows), "tp")
        parts = run_experts(pieces, gate_weight, up_weight, down_weight, slots)
        returned.append(exchange(add_up(parts)))
    return vmem_call(
        lambda *r: finish_body(chunks, *r),
        jax.ShapeDtypeStruct(residual.shape, bf16),
        operands=4 + 2 * chunks,
        name="finish",
    )(
        route_logits,
        hidden_in,
        ln2_gain[None],
        ln2_bias[None],
        *[a.reshape(-1, 1) for a in aims],
        *returned,
    )


def solution(mesh):
    nz, nx, nc = 8, 4, 2
    mesh = Mesh(mesh.devices.reshape(nz, nx, nc, mesh.shape["tp"]), ("z", "x", "c", "tp"))
    in_specs = (
        P(SP, "tp"),
        P(SP, "tp"),
        P(SP, "tp"),
        P("tp"),
        P(),
        P("tp", None),
        P((*SP, "tp"), None),
        P(),
        P(),
        P((*SP, "tp"), None),
        P((*SP, "tp"), None),
        P(SP, None, "tp"),
        P(SP, None, "tp"),
        P(SP, "tp", None),
        P(),
        P(),
    )
    out_specs = P((*SP, "tp"), None)
    return jax.shard_map(
        on_device, mesh=mesh, in_specs=in_specs, out_specs=out_specs, check_vma=False
    )
```

```python
import jax
import jax.numpy as jnp
from jax import lax
from jax.experimental import pallas as pl
from jax.experimental.pallas import tpu as pltpu
from jax.sharding import Mesh
from jax.sharding import PartitionSpec as P

residual_scale = 8.0**0.25
norm_eps = 1e-05
head_eps = 1e-06


f32 = jnp.float32
bf16 = jnp.bfloat16
LOG2E = 1.4426950408889634
SUB = 8
LANES = 128
SPOT = 16
EXTRA = 16


def shift(x, axis, step, size, wrap=True):
    pairs = [(i, (i + step) % size) for i in range(size) if wrap or 0 <= i + step < size]
    return lax.ppermute(x, axis, pairs)


def vmem_call(body, out_shape, scratch=(), smem=0, operands=0, **kw):
    specs = [pl.BlockSpec(memory_space=pltpu.SMEM)] * smem
    specs += [pl.BlockSpec(memory_space=pltpu.VMEM)] * (operands - smem)
    return pl.pallas_call(
        body,
        out_shape=out_shape,
        in_specs=specs,
        out_specs=jax.tree.map(lambda _: pl.BlockSpec(memory_space=pltpu.VMEM), out_shape),
        scratch_shapes=list(scratch),
        compiler_params=pltpu.CompilerParams(vmem_limit_bytes=56 * 1024 * 1024),
        **kw,
    )


def pack_body(k_ref, v_ref, out_ref):
    rows = k_ref.shape[0]
    heads = k_ref.shape[1] // LANES
    per = rows // SUB
    r = lax.broadcasted_iota(jnp.int32, (rows, rows), 0)
    s = lax.broadcasted_iota(jnp.int32, (rows, rows), 1)
    pick = ((r % SUB) * per + r // SUB == s).astype(f32).astype(bf16)
    ks = jnp.dot(pick, k_ref[...], preferred_element_type=f32).astype(bf16)
    vs = jnp.dot(pick, v_ref[...], preferred_element_type=f32)
    for h in range(heads):
        out_ref[h, 0:rows, :] = ks[:, h * LANES : (h + 1) * LANES]
        for p in range(rows // LANES):
            part = vs[p * LANES : (p + 1) * LANES, h * LANES : (h + 1) * LANES]
            out_ref[h, rows + p * LANES : rows + (p + 1) * LANES, :] = part.T.astype(bf16)


def attend_body(near, far, nz, nx, nc, off_ref, meta_ref, *refs):
    span = far - near
    q_refs, refs = refs[:span], refs[span:]
    own_refs, refs = refs[:nx], refs[nx:]
    twin_refs, refs = refs[:nx], refs[nx:]
    p_refs, (kv, qs, ps, acc, surv, first, second, late) = refs[:span], refs[span:]
    z, x, c = meta_ref[0], meta_ref[1], meta_ref[2]
    own_block = x * nc + c
    blocks = nx * nc
    rows = qs.shape[3]
    heads = qs.shape[1]
    scale = LANES ** (-0.5) * LOG2E
    for r in range(nx):
        at = (x + (nx - r)) % nx
        kv[at * nc + c] = own_refs[r][...]
        kv[at * nc + (1 - c)] = twin_refs[r][...]
    for s in range(span):
        for h in range(heads):
            qs[s, h] = q_refs[s][:, h * LANES : (h + 1) * LANES].astype(f32).T.astype(bf16)
    sub = lax.broadcasted_iota(jnp.int32, (SUB, LANES), 0)
    lane = lax.broadcasted_iota(jnp.int32, (SUB, LANES), 1)
    per = rows // SUB

    def score(j, s, h):
        return jnp.dot(kv[j, h, 0:rows, :], qs[s, h], preferred_element_type=f32)

    def weigh(scores, h, masked):
        offset = off_ref[h] * LOG2E
        columns = []
        for p in range(rows // LANES):
            run = jnp.zeros((SUB, LANES), f32)
            logs = [None] * per
            for i in reversed(range(per)):
                part = scores[i * SUB : (i + 1) * SUB, p * LANES : (p + 1) * LANES]
                v = part * scale - offset
                drop = jnp.maximum(v, lax.log2(1.0 + lax.exp2(jnp.minimum(v, 80.0))))
                if masked:
                    seen = sub * per + i < lane + p * LANES
                    drop = jnp.where(seen, drop, 0.0)
                run = run + drop
                logs[i] = v - run
                if masked:
                    logs[i] = jnp.where(seen, logs[i], -1e30)
            tail = run
            for d in (1, 2, 4):
                tail = tail + jnp.where(sub < SUB - d, pltpu.roll(tail, SUB - d, 0), 0.0)
            before = surv[h, :, p * LANES : (p + 1) * LANES]
            base = before + jnp.where(sub < SUB - 1, pltpu.roll(tail, SUB - 1, 0), 0.0)
            weights = jnp.concatenate([lax.exp2(u - base) for u in logs], axis=0)
            columns.append(weights.astype(bf16))
            surv[h, :, p * LANES : (p + 1) * LANES] = before + jnp.broadcast_to(
                tail[0:1], (SUB, LANES)
            )
        return jnp.concatenate(columns, axis=1)

    def add_values(j, h, weights):
        vt = jnp.concatenate(
            [
                kv[j, h, rows + p * LANES : rows + (p + 1) * LANES, :]
                for p in range(rows // LANES)
            ],
            axis=1,
        )
        acc[h] += jnp.dot(vt, weights, preferred_element_type=f32)

    def one(s, _):
        acc[...] = jnp.zeros_like(acc)
        surv[...] = jnp.zeros_like(surv)
        late[...] = jnp.zeros_like(late)

        if near == 0:

            @pl.when(s == 0)
            def _():
                for h in range(heads):
                    add_values(own_block, h, weigh(score(own_block, s, h), h, True))

            count = jnp.where(s == 0, own_block, blocks)
        else:
            count = blocks

        first[...] = score(jnp.maximum(count - 1, 0), s, 0)

        def turn(k, _):
            j = count - 1 - k
            second[...] = score(j, s, 1)
            add_values(jnp.minimum(j + 1, blocks - 1), 1, late[...])
            weights = weigh(first, 0, False)
            first[...] = score(jnp.maximum(j - 1, 0), s, 0)
            add_values(j, 0, weights)
            late[...] = weigh(second, 1, False)
            return 0

        lax.fori_loop(0, count, turn, 0)
        add_values(0, 1, late[...])
        for h in range(heads):
            ps[s, h, 0:LANES, :] = acc[h].astype(bf16)
            total = surv[h]
            high = total.astype(bf16).astype(f32)
            mid = (total - high).astype(bf16).astype(f32)
            low = total - high - mid
            wide = lax.broadcasted_iota(jnp.int32, total.shape, 0)
            split = jnp.where(
                wide == 0, high, jnp.where(wide == 1, mid, jnp.where(wide == 2, low, 0.0))
            )
            ps[s, h, LANES : LANES + EXTRA, :] = jnp.concatenate(
                [split, jnp.zeros_like(split)], axis=0
            ).astype(bf16)
        return 0

    valid = jnp.clip(nz - z - near, 0, span)
    lax.fori_loop(0, valid, one, 0)
    for s in range(span):

        @pl.when(s < valid)
        def _():
            p_refs[s][...] = ps[s]

        @pl.when(s >= valid)
        def _():
            p_refs[s][...] = jnp.zeros_like(p_refs[s])


def join_body(nz, ntp, meta_ref, *refs):
    p_refs, gain_ref, refs = refs[:nz], refs[nz], refs[nz + 1 :]
    out_refs, (whole,) = refs[:ntp], refs[ntp:]
    y = meta_ref[3]
    heads, _, rows = p_refs[0].shape
    for h in range(heads):
        total = jnp.zeros((LANES, rows), f32)
        gone = jnp.zeros((1, rows), f32)
        for s in range(nz):
            total = total + p_refs[s][h, 0:LANES, :].astype(f32) * lax.exp2(-gone)
            split = p_refs[s][h, LANES : LANES + EXTRA, :].astype(f32)
            gone = gone + jnp.sum(split, axis=0, keepdims=True)
        square = jnp.mean(total * total, axis=0, keepdims=True)
        normed = total * lax.rsqrt(square + head_eps) * gain_ref[...]
        whole[:, h * LANES : (h + 1) * LANES] = normed.T
    count = rows // ntp
    for s in range(ntp):
        at = pl.multiple_of(((y + s) % ntp) * count, count)
        out_refs[s][...] = whole[pl.ds(at, count), :].astype(bf16)


def norm_rows(value, gain, bias):
    mean = jnp.mean(value, axis=-1, keepdims=True)
    centred = value - mean
    variance = jnp.mean(centred * centred, axis=-1, keepdims=True)
    return centred * lax.rsqrt(variance + norm_eps) * gain + bias


def mix_body(chunks, a0, a1, a2, a3, w0, w1, w2a, w2b, w3, res_ref, gain_ref, bias_ref, *refs):
    target_refs, (hidden_ref, *send_refs) = refs[:chunks], refs[chunks:]
    half = w2a.shape[0]
    dot = lambda a, w: jnp.dot(a, w[...], preferred_element_type=f32)
    mixed = dot(a0[...], w0) + dot(a1[...], w1) + dot(a3[...], w3)
    mixed = mixed + dot(a2[:, :half], w2a) + dot(a2[:, half:], w2b)
    value = residual_scale * res_ref[...].astype(f32) + mixed
    hidden = norm_rows(value, gain_ref[...], bias_ref[...]).astype(bf16)
    hidden_ref[...] = hidden
    for target, send in zip(target_refs, send_refs):
        count, width = send.shape
        folds = hidden.shape[1] // width
        stack = jnp.concatenate(
            [hidden[:, q * width : (q + 1) * width] for q in range(folds)], axis=0
        )
        row = lax.broadcasted_iota(jnp.int32, (count, stack.shape[0]), 0)
        pick = (row == target[0:1, :]) | (row == target[1:2, :])
        pick = jnp.where(pick, 1.0, 0.0).astype(bf16)
        send[...] = jnp.dot(pick, stack, preferred_element_type=f32).astype(bf16)


def fold_order(size, slots, turned):
    folds = SPOT // slots
    sources = size // SPOT
    axis = 1 if turned else 0
    to = lax.broadcasted_iota(jnp.int32, (size, size), axis)
    at = lax.broadcasted_iota(jnp.int32, (size, size), 1 - axis)
    q, rest = to // (sources * slots), to % (sources * slots)
    want = (rest // slots) * SPOT + q * slots + rest % slots
    return jnp.where(want == at, 1.0, 0.0).astype(bf16)


def expert_body(slots, own, left, far_top, far_bottom, right, wg_any, wu_any, wd_any, *refs):
    outs, (x, y, wg, wu, wd, sems) = refs[:7], refs[7:]
    loads = [
        pltpu.make_async_copy(src.at[0], dst, sems.at[i])
        for i, (src, dst) in enumerate(((wg_any, wg), (wu_any, wu), (wd_any, wd)))
    ]
    for load in loads:
        load.start()
    width = own.shape[1]
    folds = SPOT // slots
    group = 16 * SPOT
    kept = 16 * slots
    to_folds = fold_order(group, slots, False)
    base = 0
    for piece in (own, left, right, far_top, far_bottom):
        for g in range(piece.shape[0] // group):
            rows = jnp.dot(
                to_folds, piece[g * group : (g + 1) * group], preferred_element_type=f32
            ).astype(bf16)
            for q in range(folds):
                x[base : base + kept, q * width : (q + 1) * width] = rows[
                    q * kept : (q + 1) * kept
                ]
            base += kept
    loads[0].wait()
    loads[1].wait()
    loads[2].wait()
    step = min(512, x.shape[0])
    hidden = wg.shape[1]
    part = 256

    def turn(m, _):
        at = pl.multiple_of(m * step, step)
        rows = x[pl.ds(at, step), :]
        active = []
        for n in range(0, hidden, part):
            gate = jnp.dot(rows, wg[:, n : n + part], preferred_element_type=f32)
            up = jnp.dot(rows, wu[:, n : n + part], preferred_element_type=f32)
            active.append((gate / (1.0 + jnp.exp(-gate)) * up).astype(bf16))
        active = jnp.concatenate(active, axis=1)
        for n in range(0, x.shape[1], part):
            y[pl.ds(at, step), n : n + part] = jnp.dot(
                active, wd[:, n : n + part], preferred_element_type=f32
            ).astype(bf16)
        return 0

    lax.fori_loop(0, x.shape[0] // step, turn, 0)
    from_folds = fold_order(group, slots, True)
    base = 0
    for out in outs:
        for g in range(out.shape[0] // group):
            rows = jnp.concatenate(
                [y[base : base + kept, q * width : (q + 1) * width] for q in range(folds)], axis=0
            )
            out[g * group : (g + 1) * group] = jnp.dot(
                from_folds, rows, preferred_element_type=f32
            ).astype(bf16)
            base += kept


def total_body(own, r1a, r1b, r2a, r2b, out):
    half = r1a.shape[0]
    for i, (a, b) in enumerate(((r1a, r2a), (r1b, r2b))):
        rows = slice(i * half, (i + 1) * half)
        out[rows] = (own[rows].astype(f32) + a[...].astype(f32) + b[...].astype(f32)).astype(bf16)


def finish_body(chunks, logits_ref, hidden_ref, gain_ref, bias_ref, *refs):
    target_refs, back_refs, (out_ref,) = refs[:chunks], refs[chunks : 2 * chunks], refs[2 * chunks :]
    logits = logits_ref[...]
    top = jnp.max(logits, axis=1, keepdims=True)
    raised = jnp.exp(logits - top)
    gates = raised / jnp.sum(raised, axis=1, keepdims=True)
    count, model = hidden_ref.shape
    choices = logits.shape[1]
    routed = None
    for target, back in zip(target_refs, back_refs):
        width = back.shape[1]
        folds = model // width
        at = lax.broadcasted_iota(jnp.int32, (target.shape[0], back.shape[0]), 1)
        pick = jnp.where(at == target[...], 1.0, 0.0).astype(bf16)
        rows = jnp.dot(pick, back[...], preferred_element_type=f32)
        mine = None
        for k in range(choices):
            spread = jnp.concatenate(
                [rows[(k * folds + q) * count : (k * folds + q + 1) * count] for q in range(folds)],
                axis=1,
            )
            spread = gates[:, k : k + 1] * spread
            mine = spread if mine is None else mine + spread
        routed = mine if routed is None else routed + mine
    value = residual_scale * hidden_ref[...].astype(f32) + routed
    out_ref[...] = norm_rows(value, gain_ref[...], bias_ref[...]).astype(bf16)


def targets(expert_ids, capacity, chunks):
    count, choices = expert_ids.shape
    flat = expert_ids.T.reshape(-1)
    earlier = jnp.arange(flat.shape[0])[:, None] > jnp.arange(flat.shape[0])[None, :]
    same = flat[:, None] == flat[None, :]
    slot = jnp.sum((same & earlier).astype(jnp.int32), axis=1)
    slots = capacity // chunks
    folds = SPOT // slots
    fold = jnp.arange(folds, dtype=jnp.int32)[None, :, None]
    base = (flat * SPOT + slot % slots).reshape(choices, 1, count) + fold * slots
    part = (slot // slots).reshape(choices, 1, count)
    return [jnp.where(part == c, base, -1) for c in range(chunks)]


def spread4(x, axis):
    half = x.shape[0] // 2
    left = shift(x, axis, 1, 4)
    right = shift(x, axis, -1, 4)
    far_top = shift(left[:half], axis, 1, 4)
    far_bottom = shift(right[half:], axis, -1, 4)
    return x, left, far_top, far_bottom, right


def mixer(
    queries, keys, values, score_offset, head_gain, out_weight, residual, gain, bias, aims, experts
):
    nz, nx, nc, ntp = (lax.axis_size(a) for a in ("z", "x", "c", "tp"))
    rows = queries.shape[0]
    heads = queries.shape[1] // LANES
    sds = jax.ShapeDtypeStruct
    slot = lax.broadcasted_iota(jnp.int32, (4,), 0)
    meta = jnp.where(
        slot == 0,
        lax.axis_index("z"),
        jnp.where(
            slot == 1,
            lax.axis_index("x"),
            jnp.where(slot == 2, lax.axis_index("c"), lax.axis_index("tp")),
        ),
    )
    packed = vmem_call(
        pack_body, sds((heads, 2 * rows, LANES), bf16), operands=2, name="pack"
    )(keys, values)
    own = [packed] + [shift(packed, "x", s, nx) for s in range(1, nx)]
    twin = [shift(o, "c", 1, nc) for o in own]
    asked = [queries] + [shift(queries, "z", -s, nz, wrap=False) for s in range(1, nz)]
    out_weight, packed = lax.optimization_barrier((out_weight, packed))
    weights = spread4(out_weight, "tp")
    partial = sds((heads, LANES + EXTRA, rows), bf16)
    back = []
    for near, far in SPANS:
        span = far - near
        if near:
            *asked, back[0] = lax.optimization_barrier((*asked, back[0]))
        parts = vmem_call(
            lambda *r: attend_body(near, far, nz, nx, nc, *r),
            [partial] * span,
            scratch=[
                pltpu.VMEM((nx * nc, heads, 2 * rows, LANES), bf16),
                pltpu.VMEM((span, heads, LANES, rows), bf16),
                pltpu.VMEM((span, heads, LANES + EXTRA, rows), bf16),
                pltpu.VMEM((heads, LANES, rows), f32),
                pltpu.VMEM((heads, SUB, rows), f32),
                pltpu.VMEM((rows, rows), f32),
                pltpu.VMEM((rows, rows), f32),
                pltpu.VMEM((rows, rows), bf16),
            ],
            smem=2,
            operands=2 + span + 2 * nx,
            cost_estimate=pl.CostEstimate(
                flops=COST * span // nz, bytes_accessed=1 << 22, transcendentals=0
            ),
            name=f"attend{near}",
        )(score_offset, meta, *asked[near:far], *own, *twin)
        back += [
            shift(p, "z", s, nz, wrap=False) if s else p for s, p in zip(range(near, far), parts)
        ]
    pieces = vmem_call(
        lambda *r: join_body(nz, ntp, *r),
        [sds((rows // ntp, heads * LANES), bf16)] * ntp,
        scratch=[pltpu.VMEM((rows, heads * LANES), f32)],
        smem=1,
        operands=2 + nz,
        name="join",
    )(meta, *back, head_gain[:, None])
    got = [pieces[0]] + [shift(pieces[s], "tp", s, ntp) for s in range(1, ntp)]
    chunks = len(aims)
    folds = aims[0].shape[1]
    width = residual.shape[1] // folds
    return vmem_call(
        lambda *r: mix_body(chunks, *r),
        [sds(residual.shape, bf16)] + [sds((experts * SPOT, width), bf16)] * chunks,
        operands=12 + chunks,
        name="mix",
    )(*got, *weights, residual, gain[None], bias[None], *[a.reshape(a.shape[0], -1) for a in aims])


def run_experts(pieces, gate_weight, up_weight, down_weight, slots):
    own = pieces[0]
    half = pieces[2]
    sds = jax.ShapeDtypeStruct
    total = sum(p.shape[0] for p in pieces) * slots // SPOT
    model, hidden = gate_weight.shape[1:]
    outs = [sds(own.shape, bf16)] + [sds(half.shape, bf16)] * 6
    vmem = pl.BlockSpec(memory_space=pltpu.VMEM)
    return pl.pallas_call(
        lambda *r: expert_body(slots, *r),
        out_shape=outs,
        in_specs=[vmem] * 5 + [pl.BlockSpec(memory_space=pl.ANY)] * 3,
        out_specs=[vmem] * 7,
        scratch_shapes=[
            pltpu.VMEM((total, model), bf16),
            pltpu.VMEM((total, model), bf16),
            pltpu.VMEM((model, hidden), bf16),
            pltpu.VMEM((model, hidden), bf16),
            pltpu.VMEM((hidden, model), bf16),
            pltpu.SemaphoreType.DMA((3,)),
        ],
        compiler_params=pltpu.CompilerParams(vmem_limit_bytes=56 * 1024 * 1024),
        name="experts",
    )(*pieces, gate_weight, up_weight, down_weight)


def add_up(parts):
    own, left_top, left_bottom, right_top, right_bottom, far_top, far_bottom = parts
    add = lambda a, b: (a.astype(f32) + b.astype(f32)).astype(bf16)
    from_left = shift(far_top, "tp", 1, 4)
    from_right = shift(far_bottom, "tp", -1, 4)
    r1b = shift(right_bottom, "tp", 1, 4)
    r2a = shift(left_top, "tp", -1, 4)
    r1a = shift(add(right_top, from_left), "tp", 1, 4)
    r2b = shift(add(left_bottom, from_right), "tp", -1, 4)
    return vmem_call(
        total_body, jax.ShapeDtypeStruct(own.shape, bf16), operands=5, name="total"
    )(own, r1a, r1b, r2a, r2b)


def exchange(rows):
    parts = rows.reshape(-1, SPOT, rows.shape[1])
    return lax.all_to_all(parts, SP, 0, 0, tiled=True).reshape(rows.shape)


SP = ("z", "x", "c")
CHUNKS = 1
SPANS = ((0, 4), (4, 8))
COST = 100_000_000_000


def on_device(
    queries,
    keys,
    values,
    score_offset,
    head_gain,
    out_weight,
    residual,
    ln1_gain,
    ln1_bias,
    expert_ids,
    route_logits,
    gate_weight,
    up_weight,
    down_weight,
    ln2_gain,
    ln2_bias,
):
    row_count = residual.shape[0]
    top_count = expert_ids.shape[1]
    experts = lax.axis_size(SP)
    capacity = max(2, 2 * top_count * row_count // experts)
    chunks = CHUNKS
    slots = capacity // chunks
    aims = targets(expert_ids, capacity, chunks)
    hidden_in, *outgoing = mixer(
        queries,
        keys,
        values,
        score_offset,
        head_gain,
        out_weight,
        residual,
        ln1_gain,
        ln1_bias,
        aims,
        experts,
    )
    returned = []
    for rows in outgoing:
        pieces = spread4(exchange(rows), "tp")
        parts = run_experts(pieces, gate_weight, up_weight, down_weight, slots)
        returned.append(exchange(add_up(parts)))
    return vmem_call(
        lambda *r: finish_body(chunks, *r),
        jax.ShapeDtypeStruct(residual.shape, bf16),
        operands=4 + 2 * chunks,
        name="finish",
    )(
        route_logits,
        hidden_in,
        ln2_gain[None],
        ln2_bias[None],
        *[a.reshape(-1, 1) for a in aims],
        *returned,
    )


def solution(mesh):
    nz, nx, nc = 8, 4, 2
    mesh = Mesh(mesh.devices.reshape(nz, nx, nc, mesh.shape["tp"]), ("z", "x", "c", "tp"))
    in_specs = (
        P(SP, "tp"),
        P(SP, "tp"),
        P(SP, "tp"),
        P("tp"),
        P(),
        P("tp", None),
        P((*SP, "tp"), None),
        P(),
        P(),
        P((*SP, "tp"), None),
        P((*SP, "tp"), None),
        P(SP, None, "tp"),
        P(SP, None, "tp"),
        P(SP, "tp", None),
        P(),
        P(),
    )
    out_specs = P((*SP, "tp"), None)
    return jax.shard_map(
        on_device, mesh=mesh, in_specs=in_specs, out_specs=out_specs, check_vma=False
    )
```

```python
import jax
import jax.numpy as jnp
from jax import lax
from jax.experimental import pallas as pl
from jax.experimental.pallas import tpu as pltpu
from jax.sharding import Mesh
from jax.sharding import PartitionSpec as P

residual_scale = 8.0**0.25
norm_eps = 1e-05
head_eps = 1e-06


f32 = jnp.float32
bf16 = jnp.bfloat16
LOG2E = 1.4426950408889634
SUB = 8
LANES = 128
SPOT = 16
EXTRA = 16


def shift(x, axis, step, size, wrap=True):
    pairs = [(i, (i + step) % size) for i in range(size) if wrap or 0 <= i + step < size]
    return lax.ppermute(x, axis, pairs)


def vmem_call(body, out_shape, scratch=(), smem=0, operands=0, **kw):
    specs = [pl.BlockSpec(memory_space=pltpu.SMEM)] * smem
    specs += [pl.BlockSpec(memory_space=pltpu.VMEM)] * (operands - smem)
    return pl.pallas_call(
        body,
        out_shape=out_shape,
        in_specs=specs,
        out_specs=jax.tree.map(lambda _: pl.BlockSpec(memory_space=pltpu.VMEM), out_shape),
        scratch_shapes=list(scratch),
        compiler_params=pltpu.CompilerParams(vmem_limit_bytes=56 * 1024 * 1024),
        **kw,
    )


def pack_body(k_ref, v_ref, out_ref):
    rows = k_ref.shape[0]
    heads = k_ref.shape[1] // LANES
    per = rows // SUB
    r = lax.broadcasted_iota(jnp.int32, (rows, rows), 0)
    s = lax.broadcasted_iota(jnp.int32, (rows, rows), 1)
    pick = ((r % SUB) * per + r // SUB == s).astype(f32).astype(bf16)
    ks = jnp.dot(pick, k_ref[...], preferred_element_type=f32).astype(bf16)
    vs = jnp.dot(pick, v_ref[...], preferred_element_type=f32)
    for h in range(heads):
        out_ref[h, 0:rows, :] = ks[:, h * LANES : (h + 1) * LANES]
        for p in range(rows // LANES):
            part = vs[p * LANES : (p + 1) * LANES, h * LANES : (h + 1) * LANES]
            out_ref[h, rows + p * LANES : rows + (p + 1) * LANES, :] = part.T.astype(bf16)


def attend_body(near, far, nz, nx, nc, off_ref, meta_ref, *refs):
    span = far - near
    q_refs, refs = refs[:span], refs[span:]
    own_refs, refs = refs[:nx], refs[nx:]
    twin_refs, refs = refs[:nx], refs[nx:]
    p_refs, (kv, qs, ps, acc, surv, first, second, late) = refs[:span], refs[span:]
    z, x, c = meta_ref[0], meta_ref[1], meta_ref[2]
    own_block = x * nc + c
    blocks = nx * nc
    rows = qs.shape[3]
    heads = qs.shape[1]
    scale = LANES ** (-0.5) * LOG2E
    for r in range(nx):
        at = (x + (nx - r)) % nx
        kv[at * nc + c] = own_refs[r][...]
        kv[at * nc + (1 - c)] = twin_refs[r][...]
    for s in range(span):
        for h in range(heads):
            qs[s, h] = q_refs[s][:, h * LANES : (h + 1) * LANES].astype(f32).T.astype(bf16)
    sub = lax.broadcasted_iota(jnp.int32, (SUB, LANES), 0)
    lane = lax.broadcasted_iota(jnp.int32, (SUB, LANES), 1)
    per = rows // SUB

    def score(j, s, h):
        return jnp.dot(kv[j, h, 0:rows, :], qs[s, h], preferred_element_type=f32)

    def weigh(scores, h, masked):
        offset = off_ref[h] * LOG2E
        columns = []
        for p in range(rows // LANES):
            run = jnp.zeros((SUB, LANES), f32)
            logs = [None] * per
            for i in reversed(range(per)):
                part = scores[i * SUB : (i + 1) * SUB, p * LANES : (p + 1) * LANES]
                v = part * scale - offset
                drop = jnp.maximum(v, lax.log2(1.0 + lax.exp2(jnp.minimum(v, 80.0))))
                if masked:
                    seen = sub * per + i < lane + p * LANES
                    drop = jnp.where(seen, drop, 0.0)
                run = run + drop
                logs[i] = v - run
                if masked:
                    logs[i] = jnp.where(seen, logs[i], -1e30)
            tail = run
            for d in (1, 2, 4):
                tail = tail + jnp.where(sub < SUB - d, pltpu.roll(tail, SUB - d, 0), 0.0)
            before = surv[h, :, p * LANES : (p + 1) * LANES]
            base = before + jnp.where(sub < SUB - 1, pltpu.roll(tail, SUB - 1, 0), 0.0)
            weights = jnp.concatenate([lax.exp2(u - base) for u in logs], axis=0)
            columns.append(weights.astype(bf16))
            surv[h, :, p * LANES : (p + 1) * LANES] = before + jnp.broadcast_to(
                tail[0:1], (SUB, LANES)
            )
        return jnp.concatenate(columns, axis=1)

    def add_values(j, h, weights):
        vt = jnp.concatenate(
            [
                kv[j, h, rows + p * LANES : rows + (p + 1) * LANES, :]
                for p in range(rows // LANES)
            ],
            axis=1,
        )
        acc[h] += jnp.dot(vt, weights, preferred_element_type=f32)

    def one(s, _):
        acc[...] = jnp.zeros_like(acc)
        surv[...] = jnp.zeros_like(surv)
        late[...] = jnp.zeros_like(late)

        if near == 0:

            @pl.when(s == 0)
            def _():
                for h in range(heads):
                    add_values(own_block, h, weigh(score(own_block, s, h), h, True))

            count = jnp.where(s == 0, own_block, blocks)
        else:
            count = blocks

        first[...] = score(jnp.maximum(count - 1, 0), s, 0)

        def turn(k, _):
            j = count - 1 - k
            second[...] = score(j, s, 1)
            add_values(jnp.minimum(j + 1, blocks - 1), 1, late[...])
            weights = weigh(first, 0, False)
            first[...] = score(jnp.maximum(j - 1, 0), s, 0)
            add_values(j, 0, weights)
            late[...] = weigh(second, 1, False)
            return 0

        lax.fori_loop(0, count, turn, 0)
        add_values(0, 1, late[...])
        for h in range(heads):
            ps[s, h, 0:LANES, :] = acc[h].astype(bf16)
            total = surv[h]
            high = total.astype(bf16).astype(f32)
            mid = (total - high).astype(bf16).astype(f32)
            low = total - high - mid
            wide = lax.broadcasted_iota(jnp.int32, total.shape, 0)
            split = jnp.where(
                wide == 0, high, jnp.where(wide == 1, mid, jnp.where(wide == 2, low, 0.0))
            )
            ps[s, h, LANES : LANES + EXTRA, :] = jnp.concatenate(
                [split, jnp.zeros_like(split)], axis=0
            ).astype(bf16)
        return 0

    valid = jnp.clip(nz - z - near, 0, span)
    lax.fori_loop(0, valid, one, 0)
    for s in range(span):

        @pl.when(s < valid)
        def _():
            p_refs[s][...] = ps[s]

        @pl.when(s >= valid)
        def _():
            p_refs[s][...] = jnp.zeros_like(p_refs[s])


def join_body(nz, ntp, meta_ref, *refs):
    p_refs, gain_ref, refs = refs[:nz], refs[nz], refs[nz + 1 :]
    out_refs, (whole,) = refs[:ntp], refs[ntp:]
    y = meta_ref[3]
    heads, _, rows = p_refs[0].shape
    for h in range(heads):
        total = jnp.zeros((LANES, rows), f32)
        gone = jnp.zeros((1, rows), f32)
        for s in range(nz):
            total = total + p_refs[s][h, 0:LANES, :].astype(f32) * lax.exp2(-gone)
            split = p_refs[s][h, LANES : LANES + EXTRA, :].astype(f32)
            gone = gone + jnp.sum(split, axis=0, keepdims=True)
        square = jnp.mean(total * total, axis=0, keepdims=True)
        normed = total * lax.rsqrt(square + head_eps) * gain_ref[...]
        whole[:, h * LANES : (h + 1) * LANES] = normed.T
    count = rows // ntp
    for s in range(ntp):
        at = pl.multiple_of(((y + s) % ntp) * count, count)
        out_refs[s][...] = whole[pl.ds(at, count), :].astype(bf16)


def norm_rows(value, gain, bias):
    mean = jnp.mean(value, axis=-1, keepdims=True)
    centred = value - mean
    variance = jnp.mean(centred * centred, axis=-1, keepdims=True)
    return centred * lax.rsqrt(variance + norm_eps) * gain + bias


def mix_body(chunks, a0, a1, a2, a3, w0, w1, w2a, w2b, w3, res_ref, gain_ref, bias_ref, *refs):
    target_refs, (hidden_ref, *send_refs) = refs[:chunks], refs[chunks:]
    half = w2a.shape[0]
    dot = lambda a, w: jnp.dot(a, w[...], preferred_element_type=f32)
    mixed = dot(a0[...], w0) + dot(a1[...], w1) + dot(a3[...], w3)
    mixed = mixed + dot(a2[:, :half], w2a) + dot(a2[:, half:], w2b)
    value = residual_scale * res_ref[...].astype(f32) + mixed
    hidden = norm_rows(value, gain_ref[...], bias_ref[...]).astype(bf16)
    hidden_ref[...] = hidden
    for target, send in zip(target_refs, send_refs):
        count, width = send.shape
        folds = hidden.shape[1] // width
        stack = jnp.concatenate(
            [hidden[:, q * width : (q + 1) * width] for q in range(folds)], axis=0
        )
        row = lax.broadcasted_iota(jnp.int32, (count, stack.shape[0]), 0)
        pick = (row == target[0:1, :]) | (row == target[1:2, :])
        pick = jnp.where(pick, 1.0, 0.0).astype(bf16)
        send[...] = jnp.dot(pick, stack, preferred_element_type=f32).astype(bf16)


def fold_order(size, slots, turned):
    folds = SPOT // slots
    sources = size // SPOT
    axis = 1 if turned else 0
    to = lax.broadcasted_iota(jnp.int32, (size, size), axis)
    at = lax.broadcasted_iota(jnp.int32, (size, size), 1 - axis)
    q, rest = to // (sources * slots), to % (sources * slots)
    want = (rest // slots) * SPOT + q * slots + rest % slots
    return jnp.where(want == at, 1.0, 0.0).astype(bf16)


def expert_body(slots, taken, given, *refs):
    pieces, (wg_any, wu_any, wd_any, *refs) = refs[:taken], refs[taken:]
    outs, (x, act, y, wg, wu, wd, sems) = refs[:given], refs[given:]
    loads = [
        pltpu.make_async_copy(src.at[0], dst, sems.at[i])
        for i, (src, dst) in enumerate(((wg_any, wg), (wu_any, wu), (wd_any, wd)))
    ]
    for load in loads:
        load.start()
    width = pieces[0].shape[1]
    folds = SPOT // slots
    group = 16 * SPOT
    kept = 16 * slots
    to_folds = fold_order(group, slots, False)
    base = 0
    for piece in pieces:
        for g in range(piece.shape[0] // group):
            rows = jnp.dot(
                to_folds, piece[g * group : (g + 1) * group], preferred_element_type=f32
            ).astype(bf16)
            for q in range(folds):
                x[base : base + kept, q * width : (q + 1) * width] = rows[
                    q * kept : (q + 1) * kept
                ]
            base += kept
    loads[0].wait()
    loads[1].wait()
    step = next(n for n in (256, 128, 64) if x.shape[0] % n == 0)
    hidden = wg.shape[1]
    part = 256

    def rise(m, _):
        at = pl.multiple_of(m * step, step)
        rows = x[pl.ds(at, step), :]
        for n in range(0, hidden, part):
            gate = jnp.dot(rows, wg[:, n : n + part], preferred_element_type=f32)
            up = jnp.dot(rows, wu[:, n : n + part], preferred_element_type=f32)
            act[pl.ds(at, step), n : n + part] = (gate / (1.0 + jnp.exp(-gate)) * up).astype(bf16)
        return 0

    def fall(m, _):
        at = pl.multiple_of(m * step, step)
        active = act[pl.ds(at, step), :]
        for n in range(0, x.shape[1], part):
            y[pl.ds(at, step), n : n + part] = jnp.dot(
                active, wd[:, n : n + part], preferred_element_type=f32
            ).astype(bf16)
        return 0

    lax.fori_loop(0, x.shape[0] // step, rise, 0)
    loads[2].wait()
    lax.fori_loop(0, x.shape[0] // step, fall, 0)
    from_folds = fold_order(group, slots, True)
    base = 0
    for out in outs:
        for g in range(out.shape[0] // group):
            rows = jnp.concatenate(
                [y[base : base + kept, q * width : (q + 1) * width] for q in range(folds)], axis=0
            )
            out[g * group : (g + 1) * group] = jnp.dot(
                from_folds, rows, preferred_element_type=f32
            ).astype(bf16)
            base += kept


def total_body(own, r1a, r1b, r2a, r2b, out):
    half = r1a.shape[0]
    for i, (a, b) in enumerate(((r1a, r2a), (r1b, r2b))):
        rows = slice(i * half, (i + 1) * half)
        out[rows] = (own[rows].astype(f32) + a[...].astype(f32) + b[...].astype(f32)).astype(bf16)


def finish_body(chunks, logits_ref, hidden_ref, gain_ref, bias_ref, *refs):
    target_refs, back_refs, (out_ref,) = refs[:chunks], refs[chunks : 2 * chunks], refs[2 * chunks :]
    logits = logits_ref[...]
    top = jnp.max(logits, axis=1, keepdims=True)
    raised = jnp.exp(logits - top)
    gates = raised / jnp.sum(raised, axis=1, keepdims=True)
    count, model = hidden_ref.shape
    choices = logits.shape[1]
    routed = None
    for target, back in zip(target_refs, back_refs):
        width = back.shape[1]
        folds = model // width
        at = lax.broadcasted_iota(jnp.int32, (target.shape[0], back.shape[0]), 1)
        pick = jnp.where(at == target[...], 1.0, 0.0).astype(bf16)
        rows = jnp.dot(pick, back[...], preferred_element_type=f32)
        mine = None
        for k in range(choices):
            spread = jnp.concatenate(
                [rows[(k * folds + q) * count : (k * folds + q + 1) * count] for q in range(folds)],
                axis=1,
            )
            spread = gates[:, k : k + 1] * spread
            mine = spread if mine is None else mine + spread
        routed = mine if routed is None else routed + mine
    value = residual_scale * hidden_ref[...].astype(f32) + routed
    out_ref[...] = norm_rows(value, gain_ref[...], bias_ref[...]).astype(bf16)


def targets(expert_ids, capacity, chunks):
    count, choices = expert_ids.shape
    flat = expert_ids.T.reshape(-1)
    earlier = jnp.arange(flat.shape[0])[:, None] > jnp.arange(flat.shape[0])[None, :]
    same = flat[:, None] == flat[None, :]
    slot = jnp.sum((same & earlier).astype(jnp.int32), axis=1)
    slots = capacity // chunks
    folds = SPOT // slots
    fold = jnp.arange(folds, dtype=jnp.int32)[None, :, None]
    base = (flat * SPOT + slot % slots).reshape(choices, 1, count) + fold * slots
    part = (slot // slots).reshape(choices, 1, count)
    return [jnp.where(part == c, base, -1) for c in range(chunks)]


def spread4(x, axis):
    half = x.shape[0] // 2
    left = shift(x, axis, 1, 4)
    right = shift(x, axis, -1, 4)
    far_top = shift(left[:half], axis, 1, 4)
    far_bottom = shift(right[half:], axis, -1, 4)
    return x, left, far_top, far_bottom, right


def mixer(
    queries, keys, values, score_offset, head_gain, out_weight, residual, gain, bias, aims, experts
):
    nz, nx, nc, ntp = (lax.axis_size(a) for a in ("z", "x", "c", "tp"))
    rows = queries.shape[0]
    heads = queries.shape[1] // LANES
    sds = jax.ShapeDtypeStruct
    slot = lax.broadcasted_iota(jnp.int32, (4,), 0)
    meta = jnp.where(
        slot == 0,
        lax.axis_index("z"),
        jnp.where(
            slot == 1,
            lax.axis_index("x"),
            jnp.where(slot == 2, lax.axis_index("c"), lax.axis_index("tp")),
        ),
    )
    packed = vmem_call(
        pack_body, sds((heads, 2 * rows, LANES), bf16), operands=2, name="pack"
    )(keys, values)
    own = [packed] + [shift(packed, "x", s, nx) for s in range(1, nx)]
    twin = [shift(o, "c", 1, nc) for o in own]
    asked = [queries] + [shift(queries, "z", -s, nz, wrap=False) for s in range(1, nz)]
    out_weight, packed = lax.optimization_barrier((out_weight, packed))
    weights = spread4(out_weight, "tp")
    partial = sds((heads, LANES + EXTRA, rows), bf16)
    found = []
    for near, far in SPANS:
        span = far - near
        if near:
            *asked, found[0] = lax.optimization_barrier((*asked, found[0]))
        parts = vmem_call(
            lambda *r: attend_body(near, far, nz, nx, nc, *r),
            [partial] * span,
            scratch=[
                pltpu.VMEM((nx * nc, heads, 2 * rows, LANES), bf16),
                pltpu.VMEM((span, heads, LANES, rows), bf16),
                pltpu.VMEM((span, heads, LANES + EXTRA, rows), bf16),
                pltpu.VMEM((heads, LANES, rows), f32),
                pltpu.VMEM((heads, SUB, rows), f32),
                pltpu.VMEM((rows, rows), f32),
                pltpu.VMEM((rows, rows), f32),
                pltpu.VMEM((rows, rows), bf16),
            ],
            smem=2,
            operands=2 + span + 2 * nx,
            cost_estimate=pl.CostEstimate(
                flops=COST * span // nz, bytes_accessed=1 << 22, transcendentals=0
            ),
            name=f"attend{near}",
        )(score_offset, meta, *asked[near:far], *own, *twin)
        found += list(parts)
    found = lax.optimization_barrier(tuple(found))
    back = [shift(p, "z", s, nz, wrap=False) if s else p for s, p in enumerate(found)]
    pieces = vmem_call(
        lambda *r: join_body(nz, ntp, *r),
        [sds((rows // ntp, heads * LANES), bf16)] * ntp,
        scratch=[pltpu.VMEM((rows, heads * LANES), f32)],
        smem=1,
        operands=2 + nz,
        name="join",
    )(meta, *back, head_gain[:, None])
    got = [pieces[0]] + [shift(pieces[s], "tp", s, ntp) for s in range(1, ntp)]
    chunks = len(aims)
    folds = aims[0].shape[1]
    width = residual.shape[1] // folds
    return vmem_call(
        lambda *r: mix_body(chunks, *r),
        [sds(residual.shape, bf16)] + [sds((experts * SPOT, width), bf16)] * chunks,
        operands=12 + chunks,
        name="mix",
    )(*got, *weights, residual, gain[None], bias[None], *[a.reshape(a.shape[0], -1) for a in aims])


def run_experts(pieces, outs, gate_weight, up_weight, down_weight, slots, name):
    total = sum(p.shape[0] for p in pieces) * slots // SPOT
    model, hidden = gate_weight.shape[1:]
    vmem = pl.BlockSpec(memory_space=pltpu.VMEM)
    return pl.pallas_call(
        lambda *r: expert_body(slots, len(pieces), len(outs), *r),
        out_shape=outs,
        in_specs=[vmem] * len(pieces) + [pl.BlockSpec(memory_space=pl.ANY)] * 3,
        out_specs=[vmem] * len(outs),
        scratch_shapes=[
            pltpu.VMEM((total, model), bf16),
            pltpu.VMEM((total, hidden), bf16),
            pltpu.VMEM((total, model), bf16),
            pltpu.VMEM((model, hidden), bf16),
            pltpu.VMEM((model, hidden), bf16),
            pltpu.VMEM((hidden, model), bf16),
            pltpu.SemaphoreType.DMA((3,)),
        ],
        compiler_params=pltpu.CompilerParams(vmem_limit_bytes=56 * 1024 * 1024),
        cost_estimate=pl.CostEstimate(
            flops=total * model * hidden * 6, bytes_accessed=1 << 24, transcendentals=0
        ),
        name=name,
    )(*pieces, gate_weight, up_weight, down_weight)


def both_runs(pieces, weights, slots):
    own, left, far_top, far_bottom, right = pieces
    whole = jax.ShapeDtypeStruct(own.shape, bf16)
    half = jax.ShapeDtypeStruct(far_top.shape, bf16)
    near = run_experts((own, left, right), [whole] + [half] * 4, *weights, slots, "experts_near")
    far = run_experts((far_top, far_bottom), [half] * 2, *weights, slots, "experts_far")
    return (*near, *far)


def add_up(parts):
    own, left_top, left_bottom, right_top, right_bottom, far_top, far_bottom = parts
    add = lambda a, b: (a.astype(f32) + b.astype(f32)).astype(bf16)
    from_left = shift(far_top, "tp", 1, 4)
    from_right = shift(far_bottom, "tp", -1, 4)
    r1b = shift(right_bottom, "tp", 1, 4)
    r2a = shift(left_top, "tp", -1, 4)
    r1a = shift(add(right_top, from_left), "tp", 1, 4)
    r2b = shift(add(left_bottom, from_right), "tp", -1, 4)
    return vmem_call(
        total_body, jax.ShapeDtypeStruct(own.shape, bf16), operands=5, name="total"
    )(own, r1a, r1b, r2a, r2b)


def exchange(rows):
    parts = rows.reshape(-1, SPOT, rows.shape[1])
    return lax.all_to_all(parts, SP, 0, 0, tiled=True).reshape(rows.shape)


SP = ("z", "x", "c")
CHUNKS = 1
SPANS = ((0, 4), (4, 8))
COST = 100_000_000_000


def on_device(
    queries,
    keys,
    values,
    score_offset,
    head_gain,
    out_weight,
    residual,
    ln1_gain,
    ln1_bias,
    expert_ids,
    route_logits,
    gate_weight,
    up_weight,
    down_weight,
    ln2_gain,
    ln2_bias,
):
    row_count = residual.shape[0]
    top_count = expert_ids.shape[1]
    experts = lax.axis_size(SP)
    capacity = max(2, 2 * top_count * row_count // experts)
    chunks = CHUNKS
    slots = capacity // chunks
    aims = targets(expert_ids, capacity, chunks)
    hidden_in, *outgoing = mixer(
        queries,
        keys,
        values,
        score_offset,
        head_gain,
        out_weight,
        residual,
        ln1_gain,
        ln1_bias,
        aims,
        experts,
    )
    returned = []
    for rows in outgoing:
        pieces = spread4(exchange(rows), "tp")
        parts = both_runs(pieces, (gate_weight, up_weight, down_weight), slots)
        returned.append(exchange(add_up(parts)))
    return vmem_call(
        lambda *r: finish_body(chunks, *r),
        jax.ShapeDtypeStruct(residual.shape, bf16),
        operands=4 + 2 * chunks,
        name="finish",
    )(
        route_logits,
        hidden_in,
        ln2_gain[None],
        ln2_bias[None],
        *[a.reshape(-1, 1) for a in aims],
        *returned,
    )


def solution(mesh):
    nz, nx, nc = 8, 4, 2
    mesh = Mesh(mesh.devices.reshape(nz, nx, nc, mesh.shape["tp"]), ("z", "x", "c", "tp"))
    in_specs = (
        P(SP, "tp"),
        P(SP, "tp"),
        P(SP, "tp"),
        P("tp"),
        P(),
        P("tp", None),
        P((*SP, "tp"), None),
        P(),
        P(),
        P((*SP, "tp"), None),
        P((*SP, "tp"), None),
        P(SP, None, "tp"),
        P(SP, None, "tp"),
        P(SP, "tp", None),
        P(),
        P(),
    )
    out_specs = P((*SP, "tp"), None)
    return jax.shard_map(
        on_device, mesh=mesh, in_specs=in_specs, out_specs=out_specs, check_vma=False
    )
```
